32 devices in a mesh: sp: 16 (over z, y, x), tp: 2 (over core).
Axes of the slice: x: 2, y: 2, z: 4, core: 2. Of those that a mesh axis runs over, the one named last changes fastest.
Arguments:
- proj_a: bfloat16 [4096, 3072], P('sp', 'tp'), may hold values from -20 to 20
- proj_gate: bfloat16 [4096, 3072], P('sp', 'tp'), may hold values from -6 to 6
- taps: bfloat16 [31, 3072], P(None, 'tp'), may hold values from -1 to 1
- norm_gain: float32 [3072], P('tp'), may hold values from 0.1 to 1.9
- norm_shift: float32 [3072], P('tp'), may hold values from -3 to 3
- cotangent: bfloat16 [4096, 3072], P('sp', 'tp'), may hold values from -6 to 6
Outputs:
- a_grad: bfloat16 [4096, 3072], P('sp', 'tp')
- gate_grad: bfloat16 [4096, 3072], P('sp', 'tp')
- taps_grad: float32 [31, 3072], P(None, 'tp')
- gain_grad: float32 [3072], P('tp')
- shift_grad: float32 [3072], P('tp')
The draws below stay inside these ranges and needn't reach their ends.
All inputs are finite; a program needn't handle non-finite values.
Results may differ from the reference program's by a relative error of at most 0.0048.
Values may be sent and summed in bfloat16 or wider, within the bound.
A program may use at most 64 MiB of HBM per device.

```python
import jax
import jax.numpy as jnp
from jax import lax

D = 3072
K = 31
TOK_DEV = 256
TOKENS = 4096
N_SP = 16


def draw_proj_a(key, part):
    first_key, second_key, third_key = jax.random.split(jax.random.fold_in(key, 17), 3)
    groups = jnp.arange(D) * 24 // D
    factors = jnp.exp(jax.random.uniform(second_key, (24,), jnp.float32, -1.1, 1.1))
    col_scale = factors[groups]
    row_groups = jnp.arange(TOKENS) * 64 // TOKENS
    row_factors = jnp.exp(jax.random.uniform(third_key, (64,), jnp.float32, -0.5, 0.5))
    row_scale = row_factors[row_groups]
    base = jax.random.truncated_normal(first_key, -4.0, 4.0, (TOKENS, D), jnp.float32)
    return (base * col_scale[None, :] * row_scale[:, None]).astype(jnp.bfloat16)


def level_of(own_key, dims, cuts, least, high):
    factor_of, own = 1.0, jax.random.fold_in(own_key, 6)
    for axis_at, parts in cuts:
        steps = jnp.exp(jax.random.uniform(jax.random.fold_in(own, axis_at), (parts,), jnp.float32, least / len(cuts), high / len(cuts)))
        factor_of = factor_of * jnp.repeat(steps, dims[axis_at] // parts).reshape([-1 if axis == axis_at else 1 for axis in range(len(dims))])
    return factor_of


def centred(key, extent, scale, most, shards=(), kind=jnp.bfloat16):
    entries = scale * jax.random.normal(key, extent, jnp.float32)
    if shards:
        entries = entries * level_of(key, extent, shards, -0.22, 0.18)
    return jnp.clip(entries, -most, most).astype(kind)


def setup_inputs(seed: int = 0) -> dict:
    key_of = jax.random.split(jax.random.key(seed), 7)
    return {
        "proj_a": draw_proj_a(jax.random.fold_in(key_of[6], 71), 0),
        "proj_gate": centred(key_of[1], (TOKENS, D), 1.5, 6.0, ((0, 16), (1, 2))),
        "taps": centred(key_of[2], (K, D), K ** -0.5, 1.0, ((1, 2),)),
        "norm_gain": jnp.clip(1.0 + 0.18 * jax.random.normal(key_of[3], (D,), jnp.float32), 0.1, 1.9),
        "norm_shift": centred(key_of[4], (D,), 0.5, 3.0, ((0, 2),), jnp.float32),
        "cotangent": centred(key_of[5], (TOKENS, D), 1.0, 6.0, ((0, 16), (1, 2))),
    }


EPS = 1e-05

def reference(proj_a, proj_gate, taps, norm_gain, norm_shift, cotangent):
    width = taps.shape[0]
    edge = width - 1
    rows = TOK_DEV
    blocks = N_SP
    gate_f = proj_gate.astype(jnp.float32)
    glu = (proj_a.astype(jnp.float32) * jax.nn.sigmoid(gate_f)).astype(jnp.bfloat16)
    glu_pad = jnp.concatenate([jnp.zeros((edge, D), jnp.bfloat16), glu], axis=0)
    tapf = taps.astype(jnp.float32)
    gain = norm_gain.astype(jnp.float32)
    shift = norm_shift.astype(jnp.float32)

    def first(index):
        start = index * rows
        ext = lax.dynamic_slice_in_dim(glu_pad, start, rows + edge, 0).astype(jnp.float32)
        cot = lax.dynamic_slice_in_dim(cotangent, start, rows, 0).astype(jnp.float32)
        conv = jnp.zeros((rows, D), jnp.float32)
        for k in range(width):
            conv = conv + tapf[k] * ext[k:k + rows]
        mean = lax.optimization_barrier(jnp.mean(conv, axis=1, keepdims=True))
        cent = conv - mean
        spread = lax.optimization_barrier(jnp.mean(cent * cent, axis=1, keepdims=True))
        rstd = lax.rsqrt(spread + EPS)
        normed = cent * rstd
        pre = normed * gain + shift
        sig = jax.nn.sigmoid(pre)
        dpre = cot * sig * (1.0 + pre * (1.0 - sig))
        dnormed = dpre * gain
        dconv = rstd * (dnormed - lax.optimization_barrier(jnp.mean(dnormed, axis=1, keepdims=True)) - normed * lax.optimization_barrier(jnp.mean(dnormed * normed, axis=1, keepdims=True)))
        return (dconv, lax.optimization_barrier(jnp.sum(dpre * normed, axis=0)), lax.optimization_barrier(jnp.sum(dpre, axis=0)))
    index = jnp.arange(blocks, dtype=jnp.int32)
    dconv_all, gain_parts, shift_parts = lax.map(first, index)
    dconv_pad = jnp.concatenate([dconv_all.reshape(blocks * rows, D), jnp.zeros((edge, D), jnp.float32)], axis=0)

    def second(index):
        start = index * rows
        dext = lax.dynamic_slice_in_dim(dconv_pad, start, rows + edge, 0)
        ext = lax.dynamic_slice_in_dim(glu_pad, start, rows + edge, 0).astype(jnp.float32)
        own = dext[:rows]
        dglu = jnp.zeros((rows, D), jnp.float32)
        for k in range(width):
            dglu = dglu + tapf[edge - k] * dext[k:k + rows]
        taps_part = jnp.stack([lax.optimization_barrier(jnp.sum(own * ext[j:j + rows], axis=0)) for j in range(width)])
        a_rows = lax.dynamic_slice_in_dim(proj_a, start, rows, 0).astype(jnp.float32)
        g_rows = lax.dynamic_slice_in_dim(gate_f, start, rows, 0)
        sg = jax.nn.sigmoid(g_rows)
        return ((dglu * sg).astype(jnp.bfloat16), (dglu * a_rows * sg * (1.0 - sg)).astype(jnp.bfloat16), taps_part)
    a_parts, gate_parts, taps_parts = lax.map(second, index)
    a_grad = a_parts.reshape(blocks * rows, D)
    gate_grad = gate_parts.reshape(blocks * rows, D)
    return (a_grad, gate_grad, lax.optimization_barrier(jnp.sum(taps_parts, axis=0)), lax.optimization_barrier(jnp.sum(gain_parts, axis=0)), lax.optimization_barrier(jnp.sum(shift_parts, axis=0)))
```

```python
import functools

import jax
import jax.numpy as jnp
from jax import lax
from jax.experimental import pallas as pl
from jax.experimental.pallas import tpu as pltpu
from jax.sharding import PartitionSpec as P

EPS = 1e-05
LANES = 128
SUB = 8
BLOCK = 64
HALO = 32
F32 = jnp.float32
BF16 = jnp.bfloat16


def plan(chans, width, n):
    tiles = chans // LANES
    group = -(-(width + 2) // SUB) * SUB
    units = tiles * (group // SUB)
    per = -(-units // n)
    owners = -(-units // per)
    return tiles, group, per * SUB, owners


def kernel(
    n, ntp, width, full,
    a_ref, g_ref, taps_ref, gain_ref, shift_ref, cot_ref,
    ag_ref, gg_ref, tg_ref, gaing_ref, shiftg_ref,
    x_s, conv_s, dn_s, d_s, taps_s, par_s,
    glu_out, glu_in, dc_out, dc_in,
    st_out, st_in, stat_s,
    red_s, rs_in, ag_src, ag_in,
    halo_send, halo_recv, st_send, st_recv,
    rs_send, rs_recv, ag_send, ag_recv,
):
    rows, chans = a_ref.shape
    edge = width - 1
    lead = HALO - edge
    tiles, group, chunk, owners = plan(chans, width, n)
    blocks = rows // BLOCK
    me = lax.axis_index("sp")
    core = lax.axis_index("tp")
    other = 1 - core

    barrier = pltpu.get_barrier_semaphore()

    def greet(step, carry):
        pl.semaphore_signal(barrier, inc=1, device_id={"sp": lax.rem(me + step, n)})
        return carry

    lax.fori_loop(1, n, greet, 0)
    pl.semaphore_signal(barrier, inc=1, device_id={"tp": other})

    def cols(j):
        return pl.ds(pl.multiple_of(j * LANES, LANES), LANES)

    def gate_tile(j, base, count):
        a = a_ref[pl.ds(base, count), cols(j)].astype(F32)
        g = g_ref[pl.ds(base, count), cols(j)].astype(F32)
        return (a * jax.nn.sigmoid(g)).astype(BF16)

    def last_rows(j, carry):
        glu_out[j] = gate_tile(j, rows - HALO, HALO)
        return carry

    lax.fori_loop(0, tiles, last_rows, 0)
    pl.semaphore_wait(barrier, n)

    glu_copy = pltpu.make_async_remote_copy(
        src_ref=glu_out, dst_ref=glu_in, send_sem=halo_send.at[0], recv_sem=halo_recv.at[0],
        device_id={"sp": lax.rem(me + 1, n)},
    )
    dc_copy = pltpu.make_async_remote_copy(
        src_ref=dc_out, dst_ref=dc_in, send_sem=halo_send.at[1], recv_sem=halo_recv.at[1],
        device_id={"sp": lax.rem(me + n - 1, n)},
    )

    @pl.when(me < n - 1)
    def _():
        glu_copy.start()

    def prepare(j, carry):
        taps_s[j, pl.ds(0, width), :] = taps_ref[:, cols(j)].astype(F32)
        par_s[j, 0:1, :] = gain_ref[:, cols(j)]
        par_s[j, 1:2, :] = shift_ref[:, cols(j)]
        for b in range(blocks):
            x_s[j, pl.ds(HALO + b * BLOCK, BLOCK), :] = gate_tile(j, b * BLOCK, BLOCK).astype(F32)
        return carry

    lax.fori_loop(0, tiles, prepare, 0)

    lane = lax.broadcasted_iota(jnp.int32, (BLOCK, LANES), 1)

    def stat_copy(i):
        return pltpu.make_async_remote_copy(
            src_ref=st_out.at[i], dst_ref=st_in.at[i], send_sem=st_send.at[i],
            recv_sem=st_recv.at[i], device_id={"tp": other},
        )

    def send_stats(i, first, second):
        first = jnp.sum(first, axis=1, keepdims=True)
        second = jnp.sum(second, axis=1, keepdims=True)
        st_out[i] = jnp.where(lane < LANES // 2, first, second)
        stat_copy(i).start()

    def both_stats(i):
        stat_copy(i).wait_recv()
        both = (st_out[i] + st_in[i]) * (1.0 / full)
        first = jnp.broadcast_to(both[:, 0:1], (BLOCK, LANES))
        second = jnp.broadcast_to(both[:, LANES // 2 : LANES // 2 + 1], (BLOCK, LANES))
        return first, second

    zero = jnp.zeros((BLOCK, LANES), F32)

    def convolve(b):
        base = b * BLOCK

        def step(j, carry):
            first, second = carry
            acc = zero
            for k in range(width):
                acc = acc + taps_s[j, k : k + 1, :] * x_s[j, pl.ds(base + lead + k, BLOCK), :]
            conv_s[j, pl.ds(base, BLOCK), :] = acc
            return first + acc, second + acc * acc

        first, second = lax.fori_loop(0, tiles, step, (zero, zero))
        send_stats(b, first, second)

    order = list(range(1, blocks)) + [0]
    for b in order[:-1]:
        convolve(b)

    @pl.when(me > 0)
    def _():
        glu_copy.wait_recv()

        def widen(j, carry):
            x_s[j, pl.ds(0, HALO), :] = glu_in[j].astype(F32)
            return carry

        lax.fori_loop(0, tiles, widen, 0)

    @pl.when(me == 0)
    def _():
        def clear(j, carry):
            x_s[j, pl.ds(0, HALO), :] = jnp.zeros((HALO, LANES), F32)
            return carry

        lax.fori_loop(0, tiles, clear, 0)

    convolve(0)

    def clear_sums(j, carry):
        par_s[j, pl.ds(SUB, 2 * SUB), :] = jnp.zeros((2 * SUB, LANES), F32)
        return carry

    lax.fori_loop(0, tiles, clear_sums, 0)

    def fold(x):
        return jnp.sum(x.reshape(x.shape[0] // SUB, SUB, LANES), axis=0)

    def normalise(b):
        base = b * BLOCK
        mean, square = both_stats(b)
        rstd = lax.rsqrt(jnp.maximum(square - mean * mean, 0.0) + EPS)
        stat_s[0, pl.ds(base, BLOCK), :] = rstd

        def step(j, carry):
            first, second = carry
            at = pl.ds(base, BLOCK)
            gain = par_s[j, 0:1, :]
            normed = (conv_s[j, at, :] - mean) * rstd
            pre = normed * gain + par_s[j, 1:2, :]
            sig = jax.nn.sigmoid(pre)
            dpre = cot_ref[at, cols(j)].astype(F32) * sig * (1.0 + pre * (1.0 - sig))
            par_s[j, pl.ds(SUB, SUB), :] += fold(dpre * normed)
            par_s[j, pl.ds(2 * SUB, SUB), :] += fold(dpre)
            dn = dpre * gain
            conv_s[j, at, :] = normed
            dn_s[j, at, :] = dn
            return first + dn, second + dn * normed

        first, second = lax.fori_loop(0, tiles, step, (zero, zero))
        send_stats(blocks + b, first, second)

    def take_stats(b):
        first, second = both_stats(blocks + b)
        at = pl.ds(b * BLOCK, BLOCK)
        stat_s[1, at, :] = first
        stat_s[2, at, :] = second

    def dconv_at(j, at):
        return stat_s[0, at, :] * (
            dn_s[j, at, :] - stat_s[1, at, :] - conv_s[j, at, :] * stat_s[2, at, :]
        )

    for b in range(blocks):
        normalise(b)
        if b == 1 or blocks == 1:
            take_stats(0)

            def head(j, carry):
                dc_out[j] = dconv_at(j, pl.ds(0, HALO)).astype(BF16)
                return carry

            lax.fori_loop(0, tiles, head, 0)

            @pl.when(me > 0)
            def _():
                dc_copy.start()

    for b in range(1, blocks):
        take_stats(b)

    def taps_step(j, carry):
        def tile(r, accs):
            base = pl.multiple_of(r * 2 * SUB, 2 * SUB)
            d = dconv_at(j, pl.ds(base, 2 * SUB))
            d_s[j, pl.ds(base, 2 * SUB), :] = d
            out = []
            for k in range(width):
                prod = d * x_s[j, pl.ds(base + lead + k, 2 * SUB), :]
                out.append(accs[k] + (prod[:SUB] + prod[SUB:]))
            return tuple(out)

        start = tuple(jnp.zeros((SUB, LANES), F32) for _ in range(width))
        accs = lax.fori_loop(0, rows // (2 * SUB), tile, start)
        at = pl.multiple_of(j * group, SUB)
        for k in range(width):
            red_s[pl.ds(at + k, 1), :] = jnp.sum(accs[k], axis=0, keepdims=True)
        for k in range(2):
            red_s[pl.ds(at + width + k, 1), :] = jnp.sum(
                par_s[j, pl.ds(SUB + k * SUB, SUB), :], axis=0, keepdims=True
            )
        for k in range(width + 2, group):
            red_s[pl.ds(at + k, 1), :] = jnp.zeros((1, LANES), F32)
        return carry

    lax.fori_loop(0, tiles, taps_step, 0)
    spare = owners * chunk - tiles * group
    if spare:
        red_s[pl.ds(tiles * group, spare), :] = jnp.zeros((spare, LANES), F32)

    def part(owner):
        return pl.ds(pl.multiple_of(owner * chunk, SUB), chunk)

    def rs_copy(owner, source, to):
        return pltpu.make_async_remote_copy(
            src_ref=red_s.at[part(owner)], dst_ref=rs_in.at[source],
            send_sem=rs_send.at[owner], recv_sem=rs_recv.at[source], device_id={"sp": to},
        )

    def ag_copy(owner, to):
        return pltpu.make_async_remote_copy(
            src_ref=ag_src, dst_ref=ag_in.at[part(owner)],
            send_sem=ag_send.at[to], recv_sem=ag_recv.at[owner], device_id={"sp": to},
        )

    def peers(run, limit=n):
        def step(d, carry):
            peer = lax.rem(me + d, n)
            if limit == n:
                run(peer)
            else:
                pl.when(peer < limit)(lambda: run(peer))
            return carry

        lax.fori_loop(1, n, step, 0)

    peers(lambda peer: rs_copy(peer, me, peer).start(), owners)

    def back(b):
        base = b * BLOCK

        def step(j, carry):
            acc = zero
            for k in range(width):
                acc = acc + taps_s[j, edge - k : edge - k + 1, :] * d_s[j, pl.ds(base + k, BLOCK), :]
            at = pl.ds(base, BLOCK)
            sg = jax.nn.sigmoid(g_ref[at, cols(j)].astype(F32))
            first = acc * sg
            ag_ref[at, cols(j)] = first.astype(BF16)
            gg_ref[at, cols(j)] = (first * a_ref[at, cols(j)].astype(F32) * (1.0 - sg)).astype(BF16)
            return carry

        lax.fori_loop(0, tiles, step, 0)

    for b in range(blocks - 1):
        back(b)

    @pl.when(me < owners)
    def _():
        rs_in[me] = red_s[part(me), :]
        peers(lambda peer: rs_copy(me, peer, peer).wait_recv())
        ag_src[...] = lax.fori_loop(
            1, n, lambda s, total: total + rs_in[s], rs_in[0]
        )
        peers(lambda peer: ag_copy(me, peer).start())
        ag_in[part(me), :] = ag_src[...]

    @pl.when(me < n - 1)
    def _():
        dc_copy.wait_recv()

        def widen(j, carry):
            d_s[j, pl.ds(rows, HALO), :] = dc_in[j].astype(F32)
            return carry

        lax.fori_loop(0, tiles, widen, 0)

    @pl.when(me == n - 1)
    def _():
        def clear(j, carry):
            d_s[j, pl.ds(rows, HALO), :] = jnp.zeros((HALO, LANES), F32)
            return carry

        lax.fori_loop(0, tiles, clear, 0)

    back(blocks - 1)

    peers(lambda peer: rs_copy(peer, me, peer).wait_send(), owners)

    @pl.when(me < n - 1)
    def _():
        glu_copy.wait_send()

    @pl.when(me > 0)
    def _():
        dc_copy.wait_send()

    for i in range(2 * blocks):
        stat_copy(i).wait_send()

    peers(lambda peer: ag_copy(peer, peer).wait_recv(), owners)

    def finish(j, carry):
        at = pl.multiple_of(j * group, SUB)
        tg_ref[:, cols(j)] = ag_in[pl.ds(at, width), :]
        gaing_ref[:, cols(j)] = ag_in[pl.ds(at + width, 1), :]
        shiftg_ref[:, cols(j)] = ag_in[pl.ds(at + width + 1, 1), :]
        return carry

    lax.fori_loop(0, tiles, finish, 0)

    @pl.when(me < owners)
    def _():
        peers(lambda peer: ag_copy(me, peer).wait_send())


def solution(mesh):
    n, ntp = mesh.shape["sp"], mesh.shape["tp"]

    def body(proj_a, proj_gate, taps, norm_gain, norm_shift, cotangent):
        rows, chans = proj_a.shape
        width = taps.shape[0]
        tiles, group, chunk, owners = plan(chans, width, n)
        blocks = rows // BLOCK
        vmem = pl.BlockSpec(memory_space=pltpu.VMEM)
        grads = pl.pallas_call(
            functools.partial(kernel, n, ntp, width, chans * ntp),
            out_shape=(
                jax.ShapeDtypeStruct((rows, chans), BF16),
                jax.ShapeDtypeStruct((rows, chans), BF16),
                jax.ShapeDtypeStruct((width, chans), F32),
                jax.ShapeDtypeStruct((1, chans), F32),
                jax.ShapeDtypeStruct((1, chans), F32),
            ),
            in_specs=[vmem] * 6,
            out_specs=(vmem,) * 5,
            scratch_shapes=[
                pltpu.VMEM((tiles, HALO + rows, LANES), F32),
                pltpu.VMEM((tiles, rows, LANES), F32),
                pltpu.VMEM((tiles, rows, LANES), F32),
                pltpu.VMEM((tiles, rows + HALO, LANES), F32),
                pltpu.VMEM((tiles, -(-width // SUB) * SUB, LANES), F32),
                pltpu.VMEM((tiles, 3 * SUB, LANES), F32),
                pltpu.VMEM((tiles, HALO, LANES), BF16),
                pltpu.VMEM((tiles, HALO, LANES), BF16),
                pltpu.VMEM((tiles, HALO, LANES), BF16),
                pltpu.VMEM((tiles, HALO, LANES), BF16),
                pltpu.VMEM((2 * blocks, BLOCK, LANES), F32),
                pltpu.VMEM((2 * blocks, BLOCK, LANES), F32),
                pltpu.VMEM((3, rows, LANES), F32),
                pltpu.VMEM((owners * chunk, LANES), F32),
                pltpu.VMEM((n, chunk, LANES), F32),
                pltpu.VMEM((chunk, LANES), F32),
                pltpu.VMEM((owners * chunk, LANES), F32),
                pltpu.SemaphoreType.DMA((2,)),
                pltpu.SemaphoreType.DMA((2,)),
                pltpu.SemaphoreType.DMA((2 * blocks,)),
                pltpu.SemaphoreType.DMA((2 * blocks,)),
                pltpu.SemaphoreType.DMA((n,)),
                pltpu.SemaphoreType.DMA((n,)),
                pltpu.SemaphoreType.DMA((n,)),
                pltpu.SemaphoreType.DMA((n,)),
            ],
            compiler_params=pltpu.CompilerParams(collective_id=0, has_side_effects=True),
        )(
            proj_a, proj_gate, taps, norm_gain.reshape(1, chans),
            norm_shift.reshape(1, chans), cotangent,
        )
        a_grad, gate_grad, taps_grad, gain_grad, shift_grad = grads
        return (
            a_grad, gate_grad, taps_grad, gain_grad.reshape(chans), shift_grad.reshape(chans)
        )

    placed = (P("sp", "tp"), P("sp", "tp"), P(None, "tp"), P("tp"), P("tp"), P("sp", "tp"))
    return jax.shard_map(
        body,
        mesh=mesh,
        in_specs=placed,
        out_specs=(P("sp", "tp"), P("sp", "tp"), P(None, "tp"), P("tp"), P("tp")),
        check_vma=False,
    )
```

```python
import functools

import jax
import jax.numpy as jnp
from jax import lax
from jax.experimental import pallas as pl
from jax.experimental.pallas import tpu as pltpu
from jax.sharding import PartitionSpec as P

EPS = 1e-05
LANES = 128
SUB = 8
BLOCK = 64
HALO = 32
F32 = jnp.float32
BF16 = jnp.bfloat16


PACK = 16


def plan(chans, width, n):
    tiles = chans // LANES
    rounds = 2 if tiles % 2 == 0 else 1
    group = -(-(width + 2) // SUB) * SUB
    total = tiles // rounds * group
    chunk = -(-total // (n * PACK)) * PACK
    owners = -(-total // chunk)
    return tiles, rounds, group, chunk, owners


def kernel(
    n, ntp, width, full,
    a_hbm, g_hbm, taps_hbm, gain_ref, shift_ref, cot_hbm,
    ag_ref, gg_ref, sums_ref,
    a_ref, g_ref, cot_ref, taps_ref, x_s, conv_s, dn_s, d_s, taps_s, par_s,
    glu_out, glu_in, dc_out, dc_in,
    st_out, st_in, stat_s,
    red_f, red_s, rs_in, ag_src, ag_in, in_sem,
    halo_send, halo_recv, st_send, st_recv,
    rs_send, rs_recv, ag_send, ag_recv,
):
    rows, chans = a_hbm.shape
    edge = width - 1
    lead = HALO - edge
    tiles, rounds, group, chunk, owners = plan(chans, width, n)
    part_tiles = tiles // rounds
    blocks = rows // BLOCK
    tail, body = pl.ds(rows - HALO, HALO), pl.ds(0, rows - HALO)
    loads = [
        pltpu.make_async_copy(src, dst, in_sem.at[i])
        for i, (src, dst) in enumerate((
            (g_hbm.at[tail, :], g_ref.at[tail, :]),
            (a_hbm.at[tail, :], a_ref.at[tail, :]),
            (g_hbm.at[body, :], g_ref.at[body, :]),
            (a_hbm.at[body, :], a_ref.at[body, :]),
            (taps_hbm, taps_ref),
            (cot_hbm, cot_ref),
        ))
    ]
    for load in loads:
        load.start()
    me = lax.axis_index("sp")
    core = lax.axis_index("tp")
    other = 1 - core

    barrier = pltpu.get_barrier_semaphore()

    def greet(step, carry):
        pl.semaphore_signal(barrier, inc=1, device_id={"sp": lax.rem(me + step, n)})
        return carry

    lax.fori_loop(1, n, greet, 0)
    pl.semaphore_signal(barrier, inc=1, device_id={"tp": other})

    def cols(j):
        return pl.ds(pl.multiple_of(j * LANES, LANES), LANES)

    def gate_tile(j, base, count):
        a = a_ref[pl.ds(base, count), cols(j)].astype(F32)
        g = g_ref[pl.ds(base, count), cols(j)].astype(F32)
        return (a * jax.nn.sigmoid(g)).astype(BF16)

    def last_rows(j, carry):
        glu_out[j] = gate_tile(j, rows - HALO, HALO)
        return carry

    loads[0].wait()
    loads[1].wait()
    lax.fori_loop(0, tiles, last_rows, 0)

    glu_copy = pltpu.make_async_remote_copy(
        src_ref=glu_out, dst_ref=glu_in, send_sem=halo_send.at[0], recv_sem=halo_recv.at[0],
        device_id={"sp": lax.rem(me + 1, n)},
    )
    dc_copy = pltpu.make_async_remote_copy(
        src_ref=dc_out, dst_ref=dc_in, send_sem=halo_send.at[1], recv_sem=halo_recv.at[1],
        device_id={"sp": lax.rem(me + n - 1, n)},
    )

    def prepare(j, carry):
        taps_s[j, pl.ds(0, width), :] = taps_ref[:, cols(j)].astype(F32)
        par_s[j, 0:1, :] = gain_ref[cols(j)].reshape(1, LANES)
        par_s[j, 1:2, :] = shift_ref[cols(j)].reshape(1, LANES)
        par_s[j, pl.ds(SUB, 2 * SUB), :] = jnp.zeros((2 * SUB, LANES), F32)
        for b in range(blocks):
            x_s[j, pl.ds(HALO + b * BLOCK, BLOCK), :] = gate_tile(j, b * BLOCK, BLOCK).astype(F32)
        return carry

    for load in loads[2:5]:
        load.wait()
    pl.semaphore_wait(barrier, n)

    @pl.when(me < n - 1)
    def _():
        glu_copy.start()

    lax.fori_loop(0, tiles, prepare, 0)

    lane = lax.broadcasted_iota(jnp.int32, (BLOCK, LANES), 1)

    def stat_copy(i):
        return pltpu.make_async_remote_copy(
            src_ref=st_out.at[i], dst_ref=st_in.at[i], send_sem=st_send.at[i],
            recv_sem=st_recv.at[i], device_id={"tp": other},
        )

    def send_stats(i, first, second):
        first = jnp.sum(first, axis=1, keepdims=True)
        second = jnp.sum(second, axis=1, keepdims=True)
        st_out[i] = jnp.where(lane < LANES // 2, first, second)
        stat_copy(i).start()

    def both_stats(i):
        stat_copy(i).wait_recv()
        both = (st_out[i] + st_in[i]) * (1.0 / full)
        first = jnp.broadcast_to(both[:, 0:1], (BLOCK, LANES))
        second = jnp.broadcast_to(both[:, LANES // 2 : LANES // 2 + 1], (BLOCK, LANES))
        return first, second

    zero = jnp.zeros((BLOCK, LANES), F32)

    def convolve(b):
        base = b * BLOCK

        def step(j, carry):
            first, second = carry
            acc = zero
            for k in range(width):
                acc = acc + taps_s[j, k : k + 1, :] * x_s[j, pl.ds(base + lead + k, BLOCK), :]
            conv_s[j, pl.ds(base, BLOCK), :] = acc
            return first + acc, second + acc * acc

        first, second = lax.fori_loop(0, tiles, step, (zero, zero))
        send_stats(b, first, second)

    def fold(x):
        return jnp.sum(x.reshape(x.shape[0] // SUB, SUB, LANES), axis=0)

    def normalise(b):
        base = b * BLOCK
        mean, square = both_stats(b)
        rstd = lax.rsqrt(jnp.maximum(square - mean * mean, 0.0) + EPS)
        stat_s[0, pl.ds(base, BLOCK), :] = rstd

        def step(j, carry):
            first, second = carry
            at = pl.ds(base, BLOCK)
            gain = par_s[j, 0:1, :]
            normed = (conv_s[j, at, :] - mean) * rstd
            pre = normed * gain + par_s[j, 1:2, :]
            sig = jax.nn.sigmoid(pre)
            dpre = cot_ref[at, cols(j)].astype(F32) * sig * (1.0 + pre * (1.0 - sig))
            par_s[j, pl.ds(SUB, SUB), :] += fold(dpre * normed)
            par_s[j, pl.ds(2 * SUB, SUB), :] += fold(dpre)
            dn = dpre * gain
            conv_s[j, at, :] = normed
            dn_s[j, at, :] = dn
            return first + dn, second + dn * normed

        first, second = lax.fori_loop(0, tiles, step, (zero, zero))
        send_stats(blocks + b, first, second)

    def take_stats(b):
        first, second = both_stats(blocks + b)
        at = pl.ds(b * BLOCK, BLOCK)
        stat_s[1, at, :] = first
        stat_s[2, at, :] = second

    def dconv_at(j, at):
        return stat_s[0, at, :] * (
            dn_s[j, at, :] - stat_s[1, at, :] - conv_s[j, at, :] * stat_s[2, at, :]
        )

    for b in range(1, blocks):
        convolve(b)
    loads[5].wait()
    for b in range(1, blocks):
        normalise(b)

    @pl.when(me > 0)
    def _():
        glu_copy.wait_recv()

        def widen(j, carry):
            x_s[j, pl.ds(0, HALO), :] = glu_in[j].astype(F32)
            return carry

        lax.fori_loop(0, tiles, widen, 0)

    @pl.when(me == 0)
    def _():
        def clear(j, carry):
            x_s[j, pl.ds(0, HALO), :] = jnp.zeros((HALO, LANES), F32)
            return carry

        lax.fori_loop(0, tiles, clear, 0)

    convolve(0)
    for b in range(1, blocks):
        take_stats(b)
    normalise(0)
    take_stats(0)

    def head(j, carry):
        dc_out[j] = dconv_at(j, pl.ds(0, HALO)).astype(BF16)
        return carry

    lax.fori_loop(0, tiles, head, 0)

    @pl.when(me > 0)
    def _():
        dc_copy.start()

    spare = owners * chunk - part_tiles * group

    def taps_round(h):
        def step(i, carry):
            j = h * part_tiles + i
            d = dconv_at(j, pl.ds(0, rows))
            d_s[j, pl.ds(0, rows), :] = d
            at = pl.multiple_of(i * group, SUB)
            for k in range(width):
                prod = d * x_s[j, pl.ds(lead + k, rows), :]
                red_f[pl.ds(at + k, 1), :] = jnp.sum(prod, axis=0, keepdims=True)
            for k in range(2):
                red_f[pl.ds(at + width + k, 1), :] = jnp.sum(
                    par_s[j, pl.ds(SUB + k * SUB, SUB), :], axis=0, keepdims=True
                )
            for k in range(width + 2, group):
                red_f[pl.ds(at + k, 1), :] = jnp.zeros((1, LANES), F32)
            return carry

        lax.fori_loop(0, part_tiles, step, 0)
        if spare:
            red_f[pl.ds(part_tiles * group, spare), :] = jnp.zeros((spare, LANES), F32)
        red_s[h] = red_f[...].astype(BF16)

    def part(owner):
        return pl.ds(pl.multiple_of(owner * chunk, PACK), chunk)

    def rs_copy(h, owner, source, to):
        return pltpu.make_async_remote_copy(
            src_ref=red_s.at[h, part(owner), :], dst_ref=rs_in.at[h, source],
            send_sem=rs_send.at[h * n + owner], recv_sem=rs_recv.at[h * n + source],
            device_id={"sp": to},
        )

    def ag_copy(h, owner, to):
        return pltpu.make_async_remote_copy(
            src_ref=ag_src.at[h], dst_ref=ag_in.at[h, part(owner), :],
            send_sem=ag_send.at[h * n + to], recv_sem=ag_recv.at[h * n + owner],
            device_id={"sp": to},
        )

    def peers(run, limit=n):
        def step(d, carry):
            peer = lax.rem(me + d, n)
            if limit == n:
                run(peer)
            else:
                pl.when(peer < limit)(lambda: run(peer))
            return carry

        lax.fori_loop(1, n, step, 0)

    def scatter(h):
        peers(lambda peer: rs_copy(h, peer, me, peer).start(), owners)

    def gather(h):
        @pl.when(me < owners)
        def _():
            rs_in[h, me] = red_s[h, part(me), :]
            peers(lambda peer: rs_copy(h, me, peer, peer).wait_recv())
            ag_src[h] = lax.fori_loop(
                1, n, lambda s, total: total + rs_in[h, s].astype(F32), rs_in[h, 0].astype(F32)
            ).astype(BF16)
            peers(lambda peer: ag_copy(h, me, peer).start())
            ag_in[h, part(me), :] = ag_src[h]

    for h in range(rounds):
        taps_round(h)
        scatter(h)

    def back(b):
        base = b * BLOCK

        def step(j, carry):
            acc = zero
            for k in range(width):
                acc = acc + taps_s[j, edge - k : edge - k + 1, :] * d_s[j, pl.ds(base + k, BLOCK), :]
            at = pl.ds(base, BLOCK)
            sg = jax.nn.sigmoid(g_ref[at, cols(j)].astype(F32))
            first = acc * sg
            ag_ref[at, cols(j)] = first.astype(BF16)
            gg_ref[at, cols(j)] = (first * a_ref[at, cols(j)].astype(F32) * (1.0 - sg)).astype(BF16)
            return carry

        lax.fori_loop(0, tiles, step, 0)

    back(0)
    for h in range(rounds - 1):
        gather(h)
    for b in range(1, blocks - 1):
        back(b)

    @pl.when(me < n - 1)
    def _():
        dc_copy.wait_recv()

        def widen(j, carry):
            d_s[j, pl.ds(rows, HALO), :] = dc_in[j].astype(F32)
            return carry

        lax.fori_loop(0, tiles, widen, 0)

    @pl.when(me == n - 1)
    def _():
        def clear(j, carry):
            d_s[j, pl.ds(rows, HALO), :] = jnp.zeros((HALO, LANES), F32)
            return carry

        lax.fori_loop(0, tiles, clear, 0)

    back(blocks - 1)
    gather(rounds - 1)

    for h in range(rounds):
        peers(lambda peer: rs_copy(h, peer, me, peer).wait_send(), owners)

    @pl.when(me < n - 1)
    def _():
        glu_copy.wait_send()

    @pl.when(me > 0)
    def _():
        dc_copy.wait_send()

    for i in range(2 * blocks):
        stat_copy(i).wait_send()

    for h in range(rounds):
        peers(lambda peer: ag_copy(h, peer, peer).wait_recv(), owners)
        sums_ref[h] = ag_in[h].astype(F32)

    @pl.when(me < owners)
    def _():
        for h in range(rounds):
            peers(lambda peer: ag_copy(h, me, peer).wait_send())


def finish(width, part_tiles, group, ag_ref, gg_ref, sums_ref, ag_out, gg_out, tg_ref, gaing_ref, shiftg_ref, sems):
    first = pltpu.make_async_copy(ag_ref, ag_out, sems.at[0])
    second = pltpu.make_async_copy(gg_ref, gg_out, sems.at[1])
    first.start()
    second.start()
    for h in range(sums_ref.shape[0]):
        for i in range(part_tiles):
            at = pl.ds((h * part_tiles + i) * LANES, LANES)
            tg_ref[:, at] = sums_ref[h, pl.ds(i * group, width), :]
            gaing_ref[at] = sums_ref[h, i * group + width, :]
            shiftg_ref[at] = sums_ref[h, i * group + width + 1, :]
    first.wait()
    second.wait()


def solution(mesh):
    n, ntp = mesh.shape["sp"], mesh.shape["tp"]

    def body(proj_a, proj_gate, taps, norm_gain, norm_shift, cotangent):
        rows, chans = proj_a.shape
        width = taps.shape[0]
        tiles, rounds, group, chunk, owners = plan(chans, width, n)
        blocks = rows // BLOCK
        vmem = pl.BlockSpec(memory_space=pltpu.VMEM)
        hbm = pl.BlockSpec(memory_space=pltpu.HBM)
        wide = jax.ShapeDtypeStruct((rows, chans), BF16)
        a_grad, gate_grad, sums = pl.pallas_call(
            functools.partial(kernel, n, ntp, width, chans * ntp),
            out_shape=(wide, wide, jax.ShapeDtypeStruct((rounds, owners * chunk, LANES), F32)),
            in_specs=[hbm, hbm, hbm, vmem, vmem, hbm],
            out_specs=(vmem,) * 3,
            scratch_shapes=[
                pltpu.VMEM((rows, chans), BF16),
                pltpu.VMEM((rows, chans), BF16),
                pltpu.VMEM((rows, chans), BF16),
                pltpu.VMEM((width, chans), BF16),
                pltpu.VMEM((tiles, HALO + rows, LANES), F32),
                pltpu.VMEM((tiles, rows, LANES), F32),
                pltpu.VMEM((tiles, rows, LANES), F32),
                pltpu.VMEM((tiles, rows + HALO, LANES), F32),
                pltpu.VMEM((tiles, -(-width // SUB) * SUB, LANES), F32),
                pltpu.VMEM((tiles, 3 * SUB, LANES), F32),
                pltpu.VMEM((tiles, HALO, LANES), BF16),
                pltpu.VMEM((tiles, HALO, LANES), BF16),
                pltpu.VMEM((tiles, HALO, LANES), BF16),
                pltpu.VMEM((tiles, HALO, LANES), BF16),
                pltpu.VMEM((2 * blocks, BLOCK, LANES), F32),
                pltpu.VMEM((2 * blocks, BLOCK, LANES), F32),
                pltpu.VMEM((3, rows, LANES), F32),
                pltpu.VMEM((owners * chunk, LANES), F32),
                pltpu.VMEM((rounds, owners * chunk, LANES), BF16),
                pltpu.VMEM((rounds, n, chunk, LANES), BF16),
                pltpu.VMEM((rounds, chunk, LANES), BF16),
                pltpu.VMEM((rounds, owners * chunk, LANES), BF16),
                pltpu.SemaphoreType.DMA((6,)),
                pltpu.SemaphoreType.DMA((2,)),
                pltpu.SemaphoreType.DMA((2,)),
                pltpu.SemaphoreType.DMA((2 * blocks,)),
                pltpu.SemaphoreType.DMA((2 * blocks,)),
                pltpu.SemaphoreType.DMA((rounds * n,)),
                pltpu.SemaphoreType.DMA((rounds * n,)),
                pltpu.SemaphoreType.DMA((rounds * n,)),
                pltpu.SemaphoreType.DMA((rounds * n,)),
            ],
            compiler_params=pltpu.CompilerParams(
                collective_id=0, has_side_effects=True, vmem_limit_bytes=32 * 1024 * 1024
            ),
        )(proj_a, proj_gate, taps, norm_gain, norm_shift, cotangent)
        vector = jax.ShapeDtypeStruct((chans,), F32)
        return pl.pallas_call(
            functools.partial(finish, width, tiles // rounds, group),
            out_shape=(wide, wide, jax.ShapeDtypeStruct((width, chans), F32), vector, vector),
            in_specs=[vmem] * 3,
            out_specs=(hbm, hbm, vmem, vmem, vmem),
            scratch_shapes=[pltpu.SemaphoreType.DMA((2,))],
            compiler_params=pltpu.CompilerParams(vmem_limit_bytes=16 * 1024 * 1024),
        )(a_grad, gate_grad, sums)

    placed = (P("sp", "tp"), P("sp", "tp"), P(None, "tp"), P("tp"), P("tp"), P("sp", "tp"))
    return jax.shard_map(
        body,
        mesh=mesh,
        in_specs=placed,
        out_specs=(P("sp", "tp"), P("sp", "tp"), P(None, "tp"), P("tp"), P("tp")),
        check_vma=False,
    )
```

```python
import functools

import jax
import jax.numpy as jnp
from jax import lax
from jax.experimental import pallas as pl
from jax.experimental.pallas import tpu as pltpu
from jax.sharding import PartitionSpec as P

EPS = 1e-05
LANES = 128
SUB = 8
BLOCK = 64
HALO = 32
F32 = jnp.float32
BF16 = jnp.bfloat16


PACK = 16


def plan(chans, width, n):
    tiles = chans // LANES
    rounds = 2 if tiles % 2 == 0 else 1
    group = -(-(width + 2) // SUB) * SUB
    total = tiles // rounds * group
    chunk = -(-total // (n * PACK)) * PACK
    owners = -(-total // chunk)
    return tiles, rounds, group, chunk, owners


def kernel(
    n, ntp, width, full,
    a_hbm, g_hbm, taps_hbm, gain_ref, shift_ref, cot_hbm,
    ag_ref, gg_ref, sums_ref,
    a_ref, g_ref, cot_ref, taps_ref, x_s, conv_s, dn_s, d_s, taps_s, par_s,
    glu_out, glu_in, dc_out, dc_in,
    st_out, st_in, stat_s,
    red_f, red_s, rs_in, ag_src, ag_in, in_sem,
    halo_send, halo_recv, st_send, st_recv,
    rs_send, rs_recv, ag_send, ag_recv,
):
    rows, chans = a_hbm.shape
    edge = width - 1
    lead = HALO - edge
    tiles, rounds, group, chunk, owners = plan(chans, width, n)
    part_tiles = tiles // rounds
    blocks = rows // BLOCK
    tail, body = pl.ds(rows - HALO, HALO), pl.ds(0, rows - HALO)
    loads = [
        pltpu.make_async_copy(src, dst, in_sem.at[i])
        for i, (src, dst) in enumerate((
            (g_hbm.at[tail, :], g_ref.at[tail, :]),
            (a_hbm.at[tail, :], a_ref.at[tail, :]),
            (g_hbm.at[body, :], g_ref.at[body, :]),
            (a_hbm.at[body, :], a_ref.at[body, :]),
            (taps_hbm, taps_ref),
            (cot_hbm, cot_ref),
        ))
    ]
    for load in loads:
        load.start()
    me = lax.axis_index("sp")
    core = lax.axis_index("tp")
    other = 1 - core

    barrier = pltpu.get_barrier_semaphore()

    def greet(step, carry):
        pl.semaphore_signal(barrier, inc=1, device_id={"sp": lax.rem(me + step, n)})
        return carry

    lax.fori_loop(1, n, greet, 0)
    pl.semaphore_signal(barrier, inc=1, device_id={"tp": other})

    def cols(j):
        return pl.ds(pl.multiple_of(j * LANES, LANES), LANES)

    def gate_tile(j, base, count):
        a = a_ref[pl.ds(base, count), cols(j)].astype(F32)
        g = g_ref[pl.ds(base, count), cols(j)].astype(F32)
        return (a * jax.nn.sigmoid(g)).astype(BF16)

    def last_rows(j, carry):
        glu_out[j] = gate_tile(j, rows - HALO, HALO)
        return carry

    loads[0].wait()
    loads[1].wait()
    lax.fori_loop(0, tiles, last_rows, 0)

    glu_copy = pltpu.make_async_remote_copy(
        src_ref=glu_out, dst_ref=glu_in, send_sem=halo_send.at[0], recv_sem=halo_recv.at[0],
        device_id={"sp": lax.rem(me + 1, n)},
    )
    dc_copy = pltpu.make_async_remote_copy(
        src_ref=dc_out, dst_ref=dc_in, send_sem=halo_send.at[1], recv_sem=halo_recv.at[1],
        device_id={"sp": lax.rem(me + n - 1, n)},
    )

    def prepare(j, carry):
        taps_s[j, pl.ds(0, width), :] = taps_ref[:, cols(j)].astype(F32)
        par_s[j, 0:1, :] = gain_ref[cols(j)].reshape(1, LANES)
        par_s[j, 1:2, :] = shift_ref[cols(j)].reshape(1, LANES)
        par_s[j, pl.ds(SUB, 2 * SUB), :] = jnp.zeros((2 * SUB, LANES), F32)
        for b in range(blocks):
            x_s[j, pl.ds(HALO + b * BLOCK, BLOCK), :] = gate_tile(j, b * BLOCK, BLOCK).astype(F32)
        return carry

    for load in loads[2:5]:
        load.wait()
    pl.semaphore_wait(barrier, n)

    @pl.when(me < n - 1)
    def _():
        glu_copy.start()

    lax.fori_loop(0, tiles, prepare, 0)

    lane = lax.broadcasted_iota(jnp.int32, (BLOCK, LANES), 1)

    def stat_copy(i):
        return pltpu.make_async_remote_copy(
            src_ref=st_out.at[i], dst_ref=st_in.at[i], send_sem=st_send.at[i],
            recv_sem=st_recv.at[i], device_id={"tp": other},
        )

    def send_stats(i, first, second):
        first = jnp.sum(first, axis=1, keepdims=True)
        second = jnp.sum(second, axis=1, keepdims=True)
        st_out[i] = jnp.where(lane < LANES // 2, first, second)
        stat_copy(i).start()

    def both_stats(i):
        stat_copy(i).wait_recv()
        both = (st_out[i] + st_in[i]) * (1.0 / full)
        first = jnp.broadcast_to(both[:, 0:1], (BLOCK, LANES))
        second = jnp.broadcast_to(both[:, LANES // 2 : LANES // 2 + 1], (BLOCK, LANES))
        return first, second

    zero = jnp.zeros((BLOCK, LANES), F32)

    def convolve(b):
        base = b * BLOCK

        def step(j, carry):
            first, second = carry
            acc = zero
            for k in range(width):
                acc = acc + taps_s[j, k : k + 1, :] * x_s[j, pl.ds(base + lead + k, BLOCK), :]
            conv_s[j, pl.ds(base, BLOCK), :] = acc
            return first + acc, second + acc * acc

        first, second = lax.fori_loop(0, tiles, step, (zero, zero))
        send_stats(b, first, second)

    def fold(x):
        return jnp.sum(x.reshape(x.shape[0] // SUB, SUB, LANES), axis=0)

    def normalise(b):
        base = b * BLOCK
        mean, square = both_stats(b)
        rstd = lax.rsqrt(jnp.maximum(square - mean * mean, 0.0) + EPS)
        stat_s[0, pl.ds(base, BLOCK), :] = rstd

        def step(j, carry):
            first, second = carry
            at = pl.ds(base, BLOCK)
            gain = par_s[j, 0:1, :]
            normed = (conv_s[j, at, :] - mean) * rstd
            pre = normed * gain + par_s[j, 1:2, :]
            sig = jax.nn.sigmoid(pre)
            dpre = cot_ref[at, cols(j)].astype(F32) * sig * (1.0 + pre * (1.0 - sig))
            par_s[j, pl.ds(SUB, SUB), :] += fold(dpre * normed)
            par_s[j, pl.ds(2 * SUB, SUB), :] += fold(dpre)
            dn = dpre * gain
            conv_s[j, at, :] = normed
            dn_s[j, at, :] = dn
            return first + dn, second + dn * normed

        first, second = lax.fori_loop(0, tiles, step, (zero, zero))
        send_stats(blocks + b, first, second)

    def take_stats(b):
        first, second = both_stats(blocks + b)
        at = pl.ds(b * BLOCK, BLOCK)
        stat_s[1, at, :] = first
        stat_s[2, at, :] = second

    def dconv_at(j, at):
        return stat_s[0, at, :] * (
            dn_s[j, at, :] - stat_s[1, at, :] - conv_s[j, at, :] * stat_s[2, at, :]
        )

    for b in range(1, blocks):
        convolve(b)
    loads[5].wait()
    for b in range(1, blocks):
        normalise(b)

    @pl.when(me > 0)
    def _():
        glu_copy.wait_recv()

        def widen(j, carry):
            x_s[j, pl.ds(0, HALO), :] = glu_in[j].astype(F32)
            return carry

        lax.fori_loop(0, tiles, widen, 0)

    @pl.when(me == 0)
    def _():
        def clear(j, carry):
            x_s[j, pl.ds(0, HALO), :] = jnp.zeros((HALO, LANES), F32)
            return carry

        lax.fori_loop(0, tiles, clear, 0)

    convolve(0)
    for b in range(1, blocks):
        take_stats(b)
    normalise(0)
    take_stats(0)

    def head(j, carry):
        dc_out[j] = dconv_at(j, pl.ds(0, HALO)).astype(BF16)
        return carry

    lax.fori_loop(0, tiles, head, 0)

    @pl.when(me > 0)
    def _():
        dc_copy.start()

    spare = owners * chunk - part_tiles * group

    def taps_round(h):
        def step(i, carry):
            j = h * part_tiles + i
            d = dconv_at(j, pl.ds(0, rows))
            d_s[j, pl.ds(0, rows), :] = d
            at = pl.multiple_of(i * group, SUB)
            for k in range(width):
                prod = d * x_s[j, pl.ds(lead + k, rows), :]
                red_f[pl.ds(at + k, 1), :] = jnp.sum(prod, axis=0, keepdims=True)
            for k in range(2):
                red_f[pl.ds(at + width + k, 1), :] = jnp.sum(
                    par_s[j, pl.ds(SUB + k * SUB, SUB), :], axis=0, keepdims=True
                )
            for k in range(width + 2, group):
                red_f[pl.ds(at + k, 1), :] = jnp.zeros((1, LANES), F32)
            return carry

        lax.fori_loop(0, part_tiles, step, 0)
        if spare:
            red_f[pl.ds(part_tiles * group, spare), :] = jnp.zeros((spare, LANES), F32)
        red_s[h] = red_f[...].astype(BF16)

    def part(owner):
        return pl.ds(pl.multiple_of(owner * chunk, PACK), chunk)

    def rs_copy(h, owner, source, to):
        return pltpu.make_async_remote_copy(
            src_ref=red_s.at[h, part(owner), :], dst_ref=rs_in.at[h, source],
            send_sem=rs_send.at[h * n + owner], recv_sem=rs_recv.at[h * n + source],
            device_id={"sp": to},
        )

    def ag_copy(h, owner, to):
        return pltpu.make_async_remote_copy(
            src_ref=ag_src.at[h], dst_ref=ag_in.at[h, part(owner), :],
            send_sem=ag_send.at[h * n + to], recv_sem=ag_recv.at[h * n + owner],
            device_id={"sp": to},
        )

    def peers(run, limit=n):
        def step(d, carry):
            peer = lax.rem(me + d, n)
            if limit == n:
                run(peer)
            else:
                pl.when(peer < limit)(lambda: run(peer))
            return carry

        lax.fori_loop(1, n, step, 0)

    def scatter(h):
        peers(lambda peer: rs_copy(h, peer, me, peer).start(), owners)

    def gather(h):
        @pl.when(me < owners)
        def _():
            rs_in[h, me] = red_s[h, part(me), :]
            peers(lambda peer: rs_copy(h, me, peer, peer).wait_recv())
            ag_src[h] = lax.fori_loop(
                1, n, lambda s, total: total + rs_in[h, s].astype(F32), rs_in[h, 0].astype(F32)
            ).astype(BF16)
            peers(lambda peer: ag_copy(h, me, peer).start())
            ag_in[h, part(me), :] = ag_src[h]

    for h in range(rounds):
        taps_round(h)
        scatter(h)

    def back(b):
        base = b * BLOCK

        def step(j, carry):
            acc = zero
            for k in range(width):
                acc = acc + taps_s[j, edge - k : edge - k + 1, :] * d_s[j, pl.ds(base + k, BLOCK), :]
            at = pl.ds(base, BLOCK)
            sg = jax.nn.sigmoid(g_ref[at, cols(j)].astype(F32))
            first = acc * sg
            ag_ref[at, cols(j)] = first.astype(BF16)
            gg_ref[at, cols(j)] = (first * a_ref[at, cols(j)].astype(F32) * (1.0 - sg)).astype(BF16)
            return carry

        lax.fori_loop(0, tiles, step, 0)

    back(0)
    for h in range(rounds - 1):
        gather(h)
    for b in range(1, blocks - 1):
        back(b)

    @pl.when(me < n - 1)
    def _():
        dc_copy.wait_recv()

        def widen(j, carry):
            d_s[j, pl.ds(rows, HALO), :] = dc_in[j].astype(F32)
            return carry

        lax.fori_loop(0, tiles, widen, 0)

    @pl.when(me == n - 1)
    def _():
        def clear(j, carry):
            d_s[j, pl.ds(rows, HALO), :] = jnp.zeros((HALO, LANES), F32)
            return carry

        lax.fori_loop(0, tiles, clear, 0)

    back(blocks - 1)
    gather(rounds - 1)

    for h in range(rounds):
        peers(lambda peer: rs_copy(h, peer, me, peer).wait_send(), owners)

    @pl.when(me < n - 1)
    def _():
        glu_copy.wait_send()

    @pl.when(me > 0)
    def _():
        dc_copy.wait_send()

    for i in range(2 * blocks):
        stat_copy(i).wait_send()

    for h in range(rounds):
        peers(lambda peer: ag_copy(h, peer, peer).wait_recv(), owners)
        sums_ref[h] = ag_in[h].astype(F32)

    @pl.when(me < owners)
    def _():
        for h in range(rounds):
            peers(lambda peer: ag_copy(h, me, peer).wait_send())


def finish(width, part_tiles, group, ag_ref, gg_ref, sums_ref, ag_out, gg_out, tg_ref, gaing_ref, shiftg_ref, sems):
    first = pltpu.make_async_copy(ag_ref, ag_out, sems.at[0])
    second = pltpu.make_async_copy(gg_ref, gg_out, sems.at[1])
    first.start()
    second.start()
    for h in range(sums_ref.shape[0]):
        for i in range(part_tiles):
            at = pl.ds((h * part_tiles + i) * LANES, LANES)
            tg_ref[:, at] = sums_ref[h, pl.ds(i * group, width), :]
            gaing_ref[at] = sums_ref[h, i * group + width, :]
            shiftg_ref[at] = sums_ref[h, i * group + width + 1, :]
    first.wait()
    second.wait()


def solution(mesh):
    n, ntp = mesh.shape["sp"], mesh.shape["tp"]

    def body(proj_a, proj_gate, taps, norm_gain, norm_shift, cotangent):
        rows, chans = proj_a.shape
        width = taps.shape[0]
        tiles, rounds, group, chunk, owners = plan(chans, width, n)
        blocks = rows // BLOCK
        vmem = pl.BlockSpec(memory_space=pltpu.VMEM)
        hbm = pl.BlockSpec(memory_space=pltpu.HBM)
        wide = jax.ShapeDtypeStruct((rows, chans), BF16)
        a_grad, gate_grad, sums = pl.pallas_call(
            functools.partial(kernel, n, ntp, width, chans * ntp),
            out_shape=(wide, wide, jax.ShapeDtypeStruct((rounds, owners * chunk, LANES), F32)),
            in_specs=[hbm, hbm, hbm, vmem, vmem, hbm],
            out_specs=(vmem,) * 3,
            scratch_shapes=[
                pltpu.VMEM((rows, chans), BF16),
                pltpu.VMEM((rows, chans), BF16),
                pltpu.VMEM((rows, chans), BF16),
                pltpu.VMEM((width, chans), BF16),
                pltpu.VMEM((tiles, HALO + rows, LANES), F32),
                pltpu.VMEM((tiles, rows, LANES), F32),
                pltpu.VMEM((tiles, rows, LANES), F32),
                pltpu.VMEM((tiles, rows + HALO, LANES), F32),
                pltpu.VMEM((tiles, -(-width // SUB) * SUB, LANES), F32),
                pltpu.VMEM((tiles, 3 * SUB, LANES), F32),
                pltpu.VMEM((tiles, HALO, LANES), BF16),
                pltpu.VMEM((tiles, HALO, LANES), BF16),
                pltpu.VMEM((tiles, HALO, LANES), BF16),
                pltpu.VMEM((tiles, HALO, LANES), BF16),
                pltpu.VMEM((2 * blocks, BLOCK, LANES), F32),
                pltpu.VMEM((2 * blocks, BLOCK, LANES), F32),
                pltpu.VMEM((3, rows, LANES), F32),
                pltpu.VMEM((owners * chunk, LANES), F32),
                pltpu.VMEM((rounds, owners * chunk, LANES), BF16),
                pltpu.VMEM((rounds, n, chunk, LANES), BF16),
                pltpu.VMEM((rounds, chunk, LANES), BF16),
                pltpu.VMEM((rounds, owners * chunk, LANES), BF16),
                pltpu.SemaphoreType.DMA((6,)),
                pltpu.SemaphoreType.DMA((2,)),
                pltpu.SemaphoreType.DMA((2,)),
                pltpu.SemaphoreType.DMA((2 * blocks,)),
                pltpu.SemaphoreType.DMA((2 * blocks,)),
                pltpu.SemaphoreType.DMA((rounds * n,)),
                pltpu.SemaphoreType.DMA((rounds * n,)),
                pltpu.SemaphoreType.DMA((rounds * n,)),
                pltpu.SemaphoreType.DMA((rounds * n,)),
            ],
            compiler_params=pltpu.CompilerParams(
                collective_id=0, has_side_effects=True, vmem_limit_bytes=32 * 1024 * 1024
            ),
        )(*(
            pltpu.with_memory_space_constraint(x, pltpu.HBM)
            for x in (proj_a, proj_gate, taps, norm_gain, norm_shift, cotangent)
        ))
        vector = jax.ShapeDtypeStruct((chans,), F32)
        return pl.pallas_call(
            functools.partial(finish, width, tiles // rounds, group),
            out_shape=(wide, wide, jax.ShapeDtypeStruct((width, chans), F32), vector, vector),
            in_specs=[vmem] * 3,
            out_specs=(hbm, hbm, vmem, vmem, vmem),
            scratch_shapes=[pltpu.SemaphoreType.DMA((2,))],
            compiler_params=pltpu.CompilerParams(vmem_limit_bytes=16 * 1024 * 1024),
        )(a_grad, gate_grad, sums)

    placed = (P("sp", "tp"), P("sp", "tp"), P(None, "tp"), P("tp"), P("tp"), P("sp", "tp"))
    return jax.shard_map(
        body,
        mesh=mesh,
        in_specs=placed,
        out_specs=(P("sp", "tp"), P("sp", "tp"), P(None, "tp"), P("tp"), P("tp")),
        check_vma=False,
    )
```
